32 devices in a mesh: sp: 8 (over z, x), tp: 4 (over y, core).
Axes of the slice: x: 2, y: 2, z: 4, core: 2. Of those that a mesh axis runs over, the one named last changes fastest.
Arguments:
- tokens: bfloat16 [4, 8192, 2048], P(None, 'sp'), may hold values from -6 to 6
- norm_gain: bfloat16 [2048], replicated, may hold values from 0.099609375 to 1.8984375
- conv_value_weight: bfloat16 [2048, 1024], P('sp', 'tp'), may hold values from -0.125 to 0.125
- conv_gate_weight: bfloat16 [2048, 1024], P('sp', 'tp'), may hold values from -0.125 to 0.125
- query_weight: bfloat16 [2048, 1024], P('sp', 'tp'), may hold values from -40 to 40
- key_weight: bfloat16 [2048, 512], P('sp', 'tp'), may hold values from -1 to 1
- value_weight: bfloat16 [2048, 512], P('sp', 'tp'), may hold values from -0.125 to 0.125
- conv_taps: bfloat16 [31, 1024], P(None, 'tp'), may hold values from -1 to 1
- conv_gain: bfloat16 [1024], P('tp'), may hold values from 0.099609375 to 1.8984375
- sink_logit: float32 [16], P('tp'), may hold values from 1 to 6
- out_conv_weight: bfloat16 [1024, 2048], P('tp', 'sp'), may hold values from -0.125 to 0.125
- out_attn_weight: bfloat16 [1024, 2048], P('tp', 'sp'), may hold values from -0.125 to 0.125
Outputs:
- mixed: bfloat16 [4, 8192, 2048], P(None, ('sp', 'tp'))
- log_total: float32 [4, 16, 8192], P(None, 'tp', 'sp')
The draws below stay inside these ranges and needn't reach their ends.
All inputs are finite; a program needn't handle non-finite values.
Results may differ from the reference program's by a relative error of at most 0.015.
Values may be sent and summed in bfloat16 or wider, within the bound.
A program may use at most 128 MiB of HBM per device.

```python
import math
import jax
import jax.numpy as jnp
from jax import lax

D = 2048
CONV_CH = 1024
HEADS = 16
KV_HEADS = 8
HEAD_DIM = 64
WINDOW = 128
CONV_K = 31
SEQS = 4
SEQ = 8192


def shared_keys(key):
    drawn = jax.random.truncated_normal(jax.random.fold_in(key, 71), -6.0, 6.0, (D, KV_HEADS * HEAD_DIM), jnp.float32)
    return drawn / jnp.sqrt(jnp.float32(D))


def draw_key_weight(key, part):
    return shared_keys(key).astype(jnp.bfloat16)


def draw_query_weight(key, part):
    drawn = jax.random.truncated_normal(jax.random.fold_in(key, 73), -6.0, 6.0, (D, HEADS * HEAD_DIM), jnp.float32)
    drawn = drawn / jnp.sqrt(jnp.float32(D))
    return drawn.astype(jnp.bfloat16)


def levels(stream_key, shape, split, smallest, largest):
    def one(dim, shards_of):
        heights = jax.random.uniform(jax.random.fold_in(jax.random.fold_in(stream_key, 6), dim), (shards_of,), jnp.float32, smallest / len(split), largest / len(split))
        return jnp.repeat(jnp.exp(heights), shape[dim] // shards_of).reshape((-1,) + (1,) * (len(shape) - dim - 1))

    gain = one(*split[0])
    for cut in split[1:]:
        gain = gain * one(*cut)
    return gain


def noise(key, dims, deviation, limit, pieces=(), kind=jnp.bfloat16):
    loudness = levels(key, dims, pieces, -0.22, 0.18) if pieces else 1.0
    result = jax.random.normal(key, dims, jnp.float32) * deviation * loudness
    return jnp.minimum(jnp.maximum(result, -limit), limit).astype(kind)


def setup_inputs(seed: int = 0) -> dict:
    streams_of = jax.random.split(jax.random.key(seed), 13)
    tokens = noise(streams_of[0], (SEQS, SEQ, D), 1.0, 6.0, ((1, 8),))
    norm_gain = jnp.clip(1.0 + 0.18 * jax.random.normal(streams_of[1], (D,), jnp.float32), 0.099609375, 1.8984375).astype(jnp.bfloat16)
    conv_value_weight = noise(streams_of[2], (D, CONV_CH), D ** -0.5, 0.125, ((0, 8), (1, 4)))
    conv_gate_weight = noise(streams_of[3], (D, CONV_CH), D ** -0.5, 0.125, ((0, 8), (1, 4)))
    query_weight = draw_query_weight(jax.random.fold_in(streams_of[12], 71), 0)
    key_weight = draw_key_weight(jax.random.fold_in(streams_of[12], 71), 0)
    value_weight = noise(streams_of[6], (D, KV_HEADS * HEAD_DIM), D ** -0.5, 0.125, ((0, 8), (1, 4)))
    conv_taps = noise(streams_of[7], (CONV_K, CONV_CH), CONV_K ** -0.5, 1.0, ((1, 4),))
    conv_gain = jnp.clip(1.0 + 0.18 * jax.random.normal(streams_of[8], (CONV_CH,), jnp.float32), 0.099609375, 1.8984375).astype(jnp.bfloat16)
    sink_logit = jnp.clip(1.0 + 5.0 * jax.random.uniform(streams_of[9], (HEADS,), jnp.float32) ** levels(streams_of[9], (HEADS,), ((0, 4),), -0.2, 0.2), 1.0, 6.0)
    out_conv_weight = noise(streams_of[10], (CONV_CH, D), (CONV_CH + HEADS * HEAD_DIM) ** -0.5, 0.125, ((0, 4), (1, 8)))
    out_attn_weight = noise(streams_of[11], (HEADS * HEAD_DIM, D), (CONV_CH + HEADS * HEAD_DIM) ** -0.5, 0.125, ((0, 4), (1, 8)))
    return dict(tokens=tokens, norm_gain=norm_gain, conv_value_weight=conv_value_weight, conv_gate_weight=conv_gate_weight, query_weight=query_weight, key_weight=key_weight, value_weight=value_weight, conv_taps=conv_taps, conv_gain=conv_gain, sink_logit=sink_logit, out_conv_weight=out_conv_weight, out_attn_weight=out_attn_weight)


EPSILON = 1e-06
ROPE_BASE = 10000.0
MASK_VALUE = -1e+30

def rotate(raw, positions):
    half_dim = raw.shape[-1] // 2
    inverse = ROPE_BASE ** (-jnp.arange(half_dim, dtype=jnp.float32) / half_dim)
    angles = positions[:, None] * inverse[None, :]
    cosine = jnp.cos(angles)[None, :, None, :]
    sine = jnp.sin(angles)[None, :, None, :]
    first, second = (raw[..., :half_dim], raw[..., half_dim:])
    return jnp.concatenate([first * cosine - second * sine, first * sine + second * cosine], axis=-1)

def reference(tokens, norm_gain, conv_value_weight, conv_gate_weight, query_weight, key_weight, value_weight, conv_taps, conv_gain, sink_logit, out_conv_weight, out_attn_weight):
    seq_count, seq_len, width = tokens.shape
    floats = tokens.astype(jnp.float32)
    row_mean = floats.mean(-1, keepdims=True)
    centred = floats - row_mean
    variance = lax.optimization_barrier(jnp.mean(centred * centred, -1, keepdims=True))
    normed = (centred * lax.rsqrt(variance + EPSILON) * norm_gain.astype(jnp.float32)).astype(jnp.bfloat16)
    flat = normed.reshape(-1, width)
    conv_value = jnp.dot(flat, conv_value_weight, preferred_element_type=jnp.float32)
    conv_gate = jnp.dot(flat, conv_gate_weight, preferred_element_type=jnp.float32)
    gated = (conv_value * jax.nn.sigmoid(conv_gate)).astype(jnp.bfloat16).reshape(seq_count, seq_len, CONV_CH)
    rim = CONV_K // 2
    padded = jnp.pad(gated, ((0, 0), (rim, rim), (0, 0)))
    taps = conv_taps.astype(jnp.float32)
    filtered = jnp.zeros((seq_count, seq_len, CONV_CH), jnp.float32)
    for tap_index in range(CONV_K):
        filtered = filtered + padded[:, tap_index:tap_index + seq_len].astype(jnp.float32) * taps[tap_index]
    chan_mean = filtered.mean(-1, keepdims=True)
    chan_centred = filtered - chan_mean
    chan_var = lax.optimization_barrier(jnp.mean(chan_centred * chan_centred, -1, keepdims=True))
    conv_out = jax.nn.silu(chan_centred * lax.rsqrt(chan_var + EPSILON) * conv_gain.astype(jnp.float32))
    conv_out = conv_out.astype(jnp.bfloat16)
    group = HEADS // KV_HEADS
    positions = jnp.arange(seq_len, dtype=jnp.float32)
    query_raw = jnp.dot(flat, query_weight, preferred_element_type=jnp.float32)
    key_raw = jnp.dot(flat, key_weight, preferred_element_type=jnp.float32)
    queries = rotate(query_raw.reshape(seq_count, seq_len, HEADS, HEAD_DIM), positions).astype(jnp.bfloat16)
    queries = queries.reshape(seq_count, seq_len, KV_HEADS, group, HEAD_DIM)
    keys = rotate(key_raw.reshape(seq_count, seq_len, KV_HEADS, HEAD_DIM), positions).astype(jnp.bfloat16)
    values = jnp.dot(flat, value_weight, preferred_element_type=jnp.float32).astype(jnp.bfloat16)
    values = values.reshape(seq_count, seq_len, KV_HEADS, HEAD_DIM)
    edge = ((0, 0), (WINDOW, WINDOW), (0, 0), (0, 0))
    keys_pad = jnp.pad(keys, edge)
    values_pad = jnp.pad(values, edge)
    block_rows = math.gcd(seq_len, 512)
    span_len = block_rows + 2 * WINDOW
    score_scale = HEAD_DIM ** (-0.5)
    sink = sink_logit.astype(jnp.float32).reshape(KV_HEADS, group)[None, :, :, None]
    relative = jnp.arange(span_len)[None, :] - jnp.arange(block_rows)[:, None]
    band = (relative >= 0) & (relative <= 2 * WINDOW)

    def one_block(block):
        first_row = (block * block_rows).astype(jnp.int32)
        q_block = lax.dynamic_slice_in_dim(queries, first_row, block_rows, 1).astype(jnp.float32)
        k_block = lax.dynamic_slice_in_dim(keys_pad, first_row, span_len, 1).astype(jnp.float32)
        v_block = lax.dynamic_slice_in_dim(values_pad, first_row, span_len, 1).astype(jnp.float32)
        scores = jnp.einsum('sqkgd,spkd->skgqp', q_block, k_block) * score_scale
        key_pos = first_row - WINDOW + jnp.arange(span_len, dtype=jnp.int32)
        allowed = band & ((key_pos >= 0) & (key_pos < seq_len))[None, :]
        scores = jnp.where(allowed, scores, MASK_VALUE)
        top = jnp.maximum(scores.max(-1), sink)
        weights = jnp.exp(scores - top[..., None])
        total = weights.sum(-1) + jnp.exp(sink - top)
        probs = (weights / total[..., None]).astype(jnp.bfloat16).astype(jnp.float32)
        out = jnp.einsum('skgqp,spkd->sqkgd', probs, v_block).astype(jnp.bfloat16)
        return (out, top + jnp.log(total))
    outs, totals = lax.map(one_block, jnp.arange(seq_len // block_rows, dtype=jnp.int32))
    attn_out = jnp.moveaxis(outs, 0, 1).reshape(seq_count * seq_len, HEADS * HEAD_DIM)
    log_total = jnp.moveaxis(totals, 0, 3).reshape(seq_count, HEADS, seq_len)
    mixed = jnp.dot(conv_out.reshape(-1, CONV_CH), out_conv_weight, preferred_element_type=jnp.float32) + jnp.dot(attn_out, out_attn_weight, preferred_element_type=jnp.float32)
    return (mixed.astype(jnp.bfloat16).reshape(seq_count, seq_len, width), log_total)
```

```python
import functools
import math

import jax
import jax.numpy as jnp
from jax import lax
from jax.experimental import pallas as pl
from jax.experimental.pallas import tpu as pltpu
from jax.sharding import PartitionSpec as P

HEAD_DIM = 64
WINDOW = 128
LANES = 128
EPSILON = 1e-06
ROPE_BASE = 10000.0
MASK_VALUE = -1e30
F32 = jnp.float32
BF16 = jnp.bfloat16
VMEM_LIMIT = 60 * 1024 * 1024


def params(*semantics):
    return pltpu.CompilerParams(
        dimension_semantics=semantics, vmem_limit_bytes=VMEM_LIMIT
    )


def cost(flops, nbytes, trans=0):
    return pl.CostEstimate(flops=flops, bytes_accessed=nbytes, transcendentals=trans)


def ring_halo(value, width):
    size, length = lax.axis_size("sp"), value.shape[1]
    up = [(i, i + 1) for i in range(size - 1)]
    down = [(j, i) for i, j in up]
    before = lax.ppermute(value[:, length - width :], "sp", up)
    after = lax.ppermute(value[:, :width], "sp", down)
    return before, after


def gated_kernel(x_ref, w_ref, o_ref):
    ch = o_ref.shape[1]
    y = jnp.dot(x_ref[...], w_ref[...], preferred_element_type=F32)
    o_ref[...] = (y[:, :ch] * jax.nn.sigmoid(y[:, ch:])).astype(BF16)


def gated_proj(x, w):
    rows, width = x.shape
    ch = w.shape[1] // 2
    block = math.gcd(rows, 512)
    return pl.pallas_call(
        gated_kernel,
        grid=(rows // block,),
        in_specs=[
            pl.BlockSpec((block, width), lambda i: (i, 0)),
            pl.BlockSpec((width, 2 * ch), lambda i: (0, 0)),
        ],
        out_specs=pl.BlockSpec((block, ch), lambda i: (i, 0)),
        out_shape=jax.ShapeDtypeStruct((rows, ch), BF16),
        compiler_params=params("arbitrary"),
        cost_estimate=cost(4 * rows * width * ch, 2 * rows * width),
        name="gated_proj",
    )(x, w)


def qkv_kernel(qw, kw, x_ref, w_ref, cos_ref, sin_ref, q_ref, kv_ref):
    y = jnp.dot(x_ref[...], w_ref[...], preferred_element_type=F32)
    block = y.shape[0]
    cos, sin = cos_ref[...], sin_ref[...]
    lane = lax.broadcasted_iota(jnp.int32, (block, LANES), 1)
    low = lax.rem(lane, HEAD_DIM) < HEAD_DIM // 2
    for c in range(y.shape[1] // LANES):
        col = c * LANES
        part = y[:, col : col + LANES]
        if col < qw + kw:
            cs, sn = cos, sin
            if col + LANES > qw + kw:
                turned = lane + col < qw + kw
                cs, sn = jnp.where(turned, cs, 1.0), jnp.where(turned, sn, 0.0)
            half = HEAD_DIM // 2
            swap = jnp.where(
                low, pltpu.roll(part, LANES - half, 1), pltpu.roll(part, half, 1)
            )
            part = part * cs + swap * sn
        if col < qw:
            q_ref[:, col : col + LANES] = (part * HEAD_DIM ** (-0.5)).astype(BF16)
        else:
            kv_ref[:, col - qw : col - qw + LANES] = part.astype(BF16)


def qkv_proj(x, w, cos, sin, qw, kw):
    rows, width = x.shape
    tok = cos.shape[0]
    block = math.gcd(tok, 512)
    per_seq = tok // block
    return pl.pallas_call(
        functools.partial(qkv_kernel, qw, kw),
        grid=(rows // block,),
        in_specs=[
            pl.BlockSpec((block, width), lambda i: (i, 0)),
            pl.BlockSpec((width, w.shape[1]), lambda i: (0, 0)),
            pl.BlockSpec((block, LANES), lambda i: (i % per_seq, 0)),
            pl.BlockSpec((block, LANES), lambda i: (i % per_seq, 0)),
        ],
        out_specs=[
            pl.BlockSpec((block, qw), lambda i: (i, 0)),
            pl.BlockSpec((block, 2 * kw), lambda i: (i, 0)),
        ],
        out_shape=[
            jax.ShapeDtypeStruct((rows, qw), BF16),
            jax.ShapeDtypeStruct((rows, 2 * kw), BF16),
        ],
        compiler_params=params("arbitrary"),
        cost_estimate=cost(2 * rows * width * w.shape[1], 2 * rows * width),
        name="qkv_proj",
    )(x, w, cos, sin)


def conv_kernel(taps_n, halo, g_ref, b_ref, a_ref, t_ref, o_ref, xf):
    tok, ch = g_ref.shape[1], g_ref.shape[2]
    share = o_ref.shape[2]
    xf[0:halo] = b_ref[0].astype(F32)
    xf[halo : halo + tok] = g_ref[0].astype(F32)
    xf[halo + tok : halo + tok + halo] = a_ref[0].astype(F32)
    rows = math.gcd(share, 64)
    lead = halo - taps_n // 2

    def step(i, carry):
        base = pl.multiple_of(i * rows, rows)
        dest = base // share
        off = pl.multiple_of(lax.rem(base, share), rows)
        for lc in range(ch // LANES):
            ls = slice(lc * LANES, (lc + 1) * LANES)
            seg = xf[pl.ds(base, rows + 2 * halo), ls]
            total = None
            for r in range(8):
                part = None
                for a in range((2 * halo) // 8):
                    j = 8 * a + r - lead
                    if 0 <= j < taps_n:
                        need = rows + 8 if r else rows
                        piece = seg[8 * a : 8 * a + need] * t_ref[j : j + 1, ls]
                        part = piece if part is None else part + piece
                if part is None:
                    continue
                if r:
                    part = part[r : r + rows]
                total = part if total is None else total + part
            o_ref[dest, 0, pl.ds(off, rows), ls] = total.astype(BF16)
        return carry

    lax.fori_loop(0, tok // rows, step, 0)


def depthwise(gated, before, after, taps, tp):
    seqs, tok, ch = gated.shape
    halo = before.shape[1]
    share = tok // tp
    taps_n = taps.shape[0]
    return pl.pallas_call(
        functools.partial(conv_kernel, taps_n, halo),
        grid=(seqs,),
        in_specs=[
            pl.BlockSpec((1, tok, ch), lambda s: (s, 0, 0)),
            pl.BlockSpec((1, halo, ch), lambda s: (s, 0, 0)),
            pl.BlockSpec((1, halo, ch), lambda s: (s, 0, 0)),
            pl.BlockSpec((taps_n, ch), lambda s: (0, 0)),
        ],
        out_specs=pl.BlockSpec((tp, 1, share, ch), lambda s: (0, s, 0, 0)),
        out_shape=jax.ShapeDtypeStruct((tp, seqs, share, ch), BF16),
        scratch_shapes=[pltpu.VMEM((tok + 2 * halo, ch), F32)],
        compiler_params=params("arbitrary"),
        cost_estimate=cost(300 * seqs * tok * ch, 4 * seqs * tok * ch),
        name="depthwise",
    )(gated, before, after, taps)


def attn_kernel(
    group, sink_ref, q_ref, kv_ref, b_ref, a_ref, o_ref, l_ref, pad, kx, vt, bias
):
    tok, qw = q_ref.shape[1], q_ref.shape[2]
    kv2 = kv_ref.shape[2]
    kw = kv2 // 2
    share = o_ref.shape[2]
    heads = qw // HEAD_DIM
    rows = bias.shape[2]
    span = rows + 2 * WINDOW
    blocks = tok // rows
    length = tok + 2 * WINDOW

    @pl.when(pl.program_id(0) == 0)
    def _():
        offset = lax.axis_index("sp") * tok
        limit = tok * lax.axis_size("sp")
        key = lax.broadcasted_iota(jnp.int32, (span, rows), 0)
        rel = key - lax.broadcasted_iota(jnp.int32, (span, rows), 1)
        band = (rel >= 0) & (rel <= 2 * WINDOW)
        for b in range(blocks):
            pos = key + (offset + b * rows - WINDOW)
            ok = band & (pos >= 0) & (pos < limit)
            bias[b] = jnp.where(ok, 0.0, MASK_VALUE)

    pad[0:WINDOW] = b_ref[0]
    pad[WINDOW : WINDOW + tok] = kv_ref[0]
    pad[WINDOW + tok : length] = a_ref[0]
    lane = lax.broadcasted_iota(jnp.int32, (length, LANES), 1)
    for h in range(heads):
        at = (h * HEAD_DIM) % LANES
        src = (h // group) * HEAD_DIM
        chunk = src // LANES * LANES
        part = pad[:, chunk : chunk + LANES].astype(F32)
        shift = (at - src % LANES) % LANES
        if shift:
            part = pltpu.roll(part, shift, 1)
        keep = (lane >= at) & (lane < at + HEAD_DIM)
        kx[h] = jnp.where(keep, part, 0.0).astype(BF16)
    first = kw // LANES * LANES
    for c in range(first, kv2, LANES):
        vt[c - first : c - first + LANES] = (
            pad[:, c : c + LANES].astype(F32).T.astype(BF16)
        )

    for b in range(blocks):
        r0 = b * rows
        dest, off = r0 // share, r0 % share
        for pair in range(qw // LANES):
            q = q_ref[0, r0 : r0 + rows, pair * LANES : (pair + 1) * LANES]
            outs = []
            for h in range(pair * 2, pair * 2 + 2):
                sink = sink_ref[h]
                s = lax.dot_general(
                    kx[h, r0 : r0 + span],
                    q,
                    (((1,), (1,)), ((), ())),
                    preferred_element_type=F32,
                )
                s = s + bias[b]
                top = jnp.maximum(jnp.max(s, axis=0, keepdims=True), sink)
                e = jnp.exp(s - top)
                total = jnp.sum(e, axis=0, keepdims=True) + jnp.exp(sink - top)
                v0 = kw + (h // group) * HEAD_DIM - first
                o = jnp.dot(
                    vt[v0 : v0 + HEAD_DIM, r0 : r0 + span],
                    e.astype(BF16),
                    preferred_element_type=F32,
                )
                outs.append(o / total)
                l_ref[0, h : h + 1, r0 : r0 + rows] = top + jnp.log(total)
            both = jnp.concatenate(outs, axis=0).T
            o_ref[dest, 0, off : off + rows, pair * LANES : (pair + 1) * LANES] = (
                both.astype(BF16)
            )


def attention(q, kv, before, after, sink, tp):
    seqs, tok, qw = q.shape
    kv2 = kv.shape[2]
    kw = kv2 // 2
    heads = qw // HEAD_DIM
    group = heads // (kw // HEAD_DIM)
    share = tok // tp
    rows = math.gcd(share, 256)
    length = tok + 2 * WINDOW
    span = rows + 2 * WINDOW
    first = kw // LANES * LANES
    return pl.pallas_call(
        functools.partial(attn_kernel, group),
        grid=(seqs,),
        in_specs=[
            pl.BlockSpec(memory_space=pltpu.SMEM),
            pl.BlockSpec((1, tok, qw), lambda s: (s, 0, 0)),
            pl.BlockSpec((1, tok, kv2), lambda s: (s, 0, 0)),
            pl.BlockSpec((1, WINDOW, kv2), lambda s: (s, 0, 0)),
            pl.BlockSpec((1, WINDOW, kv2), lambda s: (s, 0, 0)),
        ],
        out_specs=[
            pl.BlockSpec((tp, 1, share, qw), lambda s: (0, s, 0, 0)),
            pl.BlockSpec((1, heads, tok), lambda s: (s, 0, 0)),
        ],
        out_shape=[
            jax.ShapeDtypeStruct((tp, seqs, share, qw), BF16),
            jax.ShapeDtypeStruct((seqs, heads, tok), F32),
        ],
        scratch_shapes=[
            pltpu.VMEM((length, kv2), BF16),
            pltpu.VMEM((heads, length, LANES), BF16),
            pltpu.VMEM((kv2 - first, length), BF16),
            pltpu.VMEM((tok // rows, span, rows), F32),
        ],
        compiler_params=params("arbitrary"),
        cost_estimate=cost(
            2000 * seqs * tok * qw, 8 * seqs * tok * qw, seqs * heads * tok * span
        ),
        name="attention",
    )(sink, q, kv, before, after)


def out_kernel(c_ref, a_ref, g_ref, w_ref, o_ref, x):
    tp, seqs, share, ch = c_ref.shape
    qw = a_ref.shape[3]
    step = ch + qw

    @pl.when(pl.program_id(0) == 0)
    def _():
        for s in range(seqs):
            parts = [c_ref[t, s].astype(F32) for t in range(tp)]
            mean = sum(p.sum(-1, keepdims=True) for p in parts) / (tp * ch)
            parts = [p - mean for p in parts]
            var = sum((p * p).sum(-1, keepdims=True) for p in parts) / (tp * ch)
            inv = lax.rsqrt(var + EPSILON)
            r = slice(s * share, (s + 1) * share)
            for t in range(tp):
                v = parts[t] * inv * g_ref[t].astype(F32)
                x[r, t * step : t * step + ch] = jax.nn.silu(v).astype(BF16)
                x[r, t * step + ch : (t + 1) * step] = a_ref[t, s]

    w = w_ref[0].reshape(tp * step, w_ref.shape[3])
    y = jnp.dot(x[...], w, preferred_element_type=F32).astype(BF16)
    o_ref[...] = y.reshape(o_ref.shape)


def out_proj(conv_tok, attn_tok, gain, weights):
    tp, seqs, share, ch = conv_tok.shape
    qw = attn_tok.shape[3]
    sp, _, depth, cols = weights.shape
    return pl.pallas_call(
        out_kernel,
        grid=(sp,),
        in_specs=[
            pl.BlockSpec((tp, seqs, share, ch), lambda j: (0, 0, 0, 0)),
            pl.BlockSpec((tp, seqs, share, qw), lambda j: (0, 0, 0, 0)),
            pl.BlockSpec((tp, 1, ch), lambda j: (0, 0, 0)),
            pl.BlockSpec((1, tp, depth, cols), lambda j: (j, 0, 0, 0)),
        ],
        out_specs=pl.BlockSpec((seqs, share, cols), lambda j: (0, 0, j)),
        out_shape=jax.ShapeDtypeStruct((seqs, share, sp * cols), BF16),
        scratch_shapes=[pltpu.VMEM((seqs * share, tp * depth), BF16)],
        compiler_params=params("arbitrary"),
        cost_estimate=cost(
            2 * seqs * share * tp * depth * sp * cols, 2 * sp * tp * depth * cols
        ),
        name="out_proj",
    )(conv_tok, attn_tok, gain, weights)


def on_device(
    tokens,
    norm_gain,
    conv_value_weight,
    conv_gate_weight,
    query_weight,
    key_weight,
    value_weight,
    conv_taps,
    conv_gain,
    sink_logit,
    out_conv_weight,
    out_attn_weight,
):
    seqs, tok, width = tokens.shape
    tp, sp = lax.axis_size("tp"), lax.axis_size("sp")
    ch = conv_value_weight.shape[1]
    qw, kw = query_weight.shape[1], key_weight.shape[1]

    conv_w = lax.all_gather(
        jnp.concatenate([conv_value_weight, conv_gate_weight], 1), "sp", axis=0, tiled=True
    )
    qkv_w = lax.all_gather(
        jnp.concatenate([query_weight, key_weight, value_weight], 1),
        "sp",
        axis=0,
        tiled=True,
    )
    out_w = lax.all_gather(
        jnp.concatenate([out_conv_weight, out_attn_weight], 0),
        ("sp", "tp"),
        axis=0,
        tiled=True,
    ).reshape(sp, tp, ch + qw, out_conv_weight.shape[1])
    gain = lax.all_gather(conv_gain.reshape(1, 1, ch), "tp", axis=0, tiled=True)

    floats = tokens.astype(F32)
    row_mean = floats.mean(-1, keepdims=True)
    centred = floats - row_mean
    variance = jnp.mean(centred * centred, -1, keepdims=True)
    normed = (centred * lax.rsqrt(variance + EPSILON) * norm_gain.astype(F32)).astype(BF16)
    normed = normed.reshape(seqs * tok, width)

    half = HEAD_DIM // 2
    lane = jnp.arange(LANES)
    inverse = ROPE_BASE ** (-(lane % half).astype(F32) / half)
    positions = (lax.axis_index("sp") * tok + jnp.arange(tok, dtype=jnp.int32)).astype(F32)
    angles = positions[:, None] * inverse[None, :]
    cos = jnp.cos(angles)
    sin = jnp.sin(angles) * jnp.where(lane % HEAD_DIM < half, -1.0, 1.0)[None, :]

    gated = gated_proj(normed, conv_w).reshape(seqs, tok, ch)
    halo = -(-(conv_taps.shape[0] // 2) // 16) * 16
    before, after = ring_halo(gated, halo)
    filtered = depthwise(gated, before, after, conv_taps.astype(F32), tp)
    conv_tok = lax.all_to_all(filtered, "tp", split_axis=0, concat_axis=0, tiled=True)

    q, kv = qkv_proj(normed, qkv_w, cos, sin, qw, kw)
    q, kv = q.reshape(seqs, tok, qw), kv.reshape(seqs, tok, 2 * kw)
    kv_before, kv_after = ring_halo(kv, WINDOW)
    attn_out, log_total = attention(q, kv, kv_before, kv_after, sink_logit, tp)
    attn_tok = lax.all_to_all(attn_out, "tp", split_axis=0, concat_axis=0, tiled=True)

    mixed = out_proj(conv_tok, attn_tok, gain, out_w)
    return (mixed, log_total)


def solution(mesh):
    placed = (
        P(None, "sp", None),
        P(),
        P("sp", "tp"),
        P("sp", "tp"),
        P("sp", "tp"),
        P("sp", "tp"),
        P("sp", "tp"),
        P(None, "tp"),
        P("tp"),
        P("tp"),
        P("tp", "sp"),
        P("tp", "sp"),
    )
    return jax.shard_map(
        on_device,
        mesh=mesh,
        in_specs=placed,
        out_specs=(P(None, ("sp", "tp"), None), P(None, "tp", "sp")),
        check_vma=False,
    )
```

```python
import functools
import math

import jax
import jax.numpy as jnp
from jax import lax
from jax.experimental import pallas as pl
from jax.experimental.pallas import tpu as pltpu
from jax.sharding import PartitionSpec as P

HEAD_DIM = 64
WINDOW = 128
LANES = 128
EPSILON = 1e-06
ROPE_BASE = 10000.0
MASK_VALUE = -1e30
F32 = jnp.float32
BF16 = jnp.bfloat16
VMEM_LIMIT = 60 * 1024 * 1024


def params(*semantics):
    return pltpu.CompilerParams(
        dimension_semantics=semantics, vmem_limit_bytes=VMEM_LIMIT
    )


def cost(flops, nbytes, trans=0):
    return pl.CostEstimate(flops=flops, bytes_accessed=nbytes, transcendentals=trans)


def ring_halo(value, width):
    size, length = lax.axis_size("sp"), value.shape[1]
    up = [(i, i + 1) for i in range(size - 1)]
    down = [(j, i) for i, j in up]
    before = lax.ppermute(value[:, length - width :], "sp", up)
    after = lax.ppermute(value[:, :width], "sp", down)
    return before, after


def proj_kernel(qw, kw, x_ref, w_ref, cos_ref, sin_ref, g_ref, q_ref, kv_ref):
    ch = g_ref.shape[1]
    x = x_ref[...]
    y = jnp.dot(x, w_ref[:, : 2 * ch], preferred_element_type=F32)
    g_ref[...] = (y[:, :ch] * jax.nn.sigmoid(y[:, ch:])).astype(BF16)
    y = jnp.dot(x, w_ref[:, 2 * ch :], preferred_element_type=F32)
    block = y.shape[0]
    cos, sin = cos_ref[...], sin_ref[...]
    lane = lax.broadcasted_iota(jnp.int32, (block, LANES), 1)
    low = lax.rem(lane, HEAD_DIM) < HEAD_DIM // 2
    for c in range(y.shape[1] // LANES):
        col = c * LANES
        part = y[:, col : col + LANES]
        if col < qw + kw:
            cs, sn = cos, sin
            if col + LANES > qw + kw:
                turned = lane + col < qw + kw
                cs, sn = jnp.where(turned, cs, 1.0), jnp.where(turned, sn, 0.0)
            half = HEAD_DIM // 2
            swap = jnp.where(
                low, pltpu.roll(part, LANES - half, 1), pltpu.roll(part, half, 1)
            )
            part = part * cs + swap * sn
        if col < qw:
            q_ref[:, col : col + LANES] = (part * HEAD_DIM ** (-0.5)).astype(BF16)
        else:
            kv_ref[:, col - qw : col - qw + LANES] = part.astype(BF16)


def projections(x, w, cos, sin, ch, qw, kw):
    rows, width = x.shape
    tok = cos.shape[0]
    block = math.gcd(tok, 512)
    per_seq = tok // block
    return pl.pallas_call(
        functools.partial(proj_kernel, qw, kw),
        grid=(rows // block,),
        in_specs=[
            pl.BlockSpec((block, width), lambda i: (i, 0)),
            pl.BlockSpec((width, w.shape[1]), lambda i: (0, 0)),
            pl.BlockSpec((block, LANES), lambda i: (i % per_seq, 0)),
            pl.BlockSpec((block, LANES), lambda i: (i % per_seq, 0)),
        ],
        out_specs=[
            pl.BlockSpec((block, ch), lambda i: (i, 0)),
            pl.BlockSpec((block, qw), lambda i: (i, 0)),
            pl.BlockSpec((block, 2 * kw), lambda i: (i, 0)),
        ],
        out_shape=[
            jax.ShapeDtypeStruct((rows, ch), BF16),
            jax.ShapeDtypeStruct((rows, qw), BF16),
            jax.ShapeDtypeStruct((rows, 2 * kw), BF16),
        ],
        compiler_params=params("arbitrary"),
        cost_estimate=cost(2 * rows * width * w.shape[1], 2 * rows * width),
        name="projections",
    )(x, w, cos, sin)


def conv_kernel(taps_n, halo, g_ref, b_ref, a_ref, t_ref, o_ref, xf):
    tok, ch = g_ref.shape[1], g_ref.shape[2]
    share = o_ref.shape[2]
    xf[0:halo] = b_ref[0].astype(F32)
    xf[halo : halo + tok] = g_ref[0].astype(F32)
    xf[halo + tok : halo + tok + halo] = a_ref[0].astype(F32)
    rows = math.gcd(share, 64)
    lead = halo - taps_n // 2

    def step(i, carry):
        base = pl.multiple_of(i * rows, rows)
        dest = base // share
        off = pl.multiple_of(lax.rem(base, share), rows)
        for lc in range(ch // LANES):
            ls = slice(lc * LANES, (lc + 1) * LANES)
            seg = xf[pl.ds(base, rows + 2 * halo), ls]
            total = None
            for r in range(8):
                part = None
                for a in range((2 * halo) // 8):
                    j = 8 * a + r - lead
                    if 0 <= j < taps_n:
                        need = rows + 8 if r else rows
                        piece = seg[8 * a : 8 * a + need] * t_ref[j : j + 1, ls]
                        part = piece if part is None else part + piece
                if part is None:
                    continue
                if r:
                    part = part[r : r + rows]
                total = part if total is None else total + part
            o_ref[dest, 0, pl.ds(off, rows), ls] = total.astype(BF16)
        return carry

    lax.fori_loop(0, tok // rows, step, 0)


def depthwise(gated, before, after, taps, tp):
    seqs, tok, ch = gated.shape
    halo = before.shape[1]
    share = tok // tp
    taps_n = taps.shape[0]
    return pl.pallas_call(
        functools.partial(conv_kernel, taps_n, halo),
        grid=(seqs,),
        in_specs=[
            pl.BlockSpec((1, tok, ch), lambda s: (s, 0, 0)),
            pl.BlockSpec((1, halo, ch), lambda s: (s, 0, 0)),
            pl.BlockSpec((1, halo, ch), lambda s: (s, 0, 0)),
            pl.BlockSpec((taps_n, ch), lambda s: (0, 0)),
        ],
        out_specs=pl.BlockSpec((tp, 1, share, ch), lambda s: (0, s, 0, 0)),
        out_shape=jax.ShapeDtypeStruct((tp, seqs, share, ch), BF16),
        scratch_shapes=[pltpu.VMEM((tok + 2 * halo, ch), F32)],
        compiler_params=params("arbitrary"),
        cost_estimate=cost(300 * seqs * tok * ch, 4 * seqs * tok * ch),
        name="depthwise",
    )(gated, before, after, taps)


def attn_kernel(
    group, sink_ref, q_ref, kv_ref, b_ref, a_ref, o_ref, l_ref, pad, kx, vt, bias
):
    tok, qw = q_ref.shape[1], q_ref.shape[2]
    kv2 = kv_ref.shape[2]
    kw = kv2 // 2
    share = o_ref.shape[2]
    heads = qw // HEAD_DIM
    rows = bias.shape[2]
    span = rows + 2 * WINDOW
    blocks = tok // rows
    length = tok + 2 * WINDOW

    @pl.when(pl.program_id(0) == 0)
    def _():
        offset = lax.axis_index("sp") * tok
        limit = tok * lax.axis_size("sp")
        key = lax.broadcasted_iota(jnp.int32, (span, rows), 0)
        rel = key - lax.broadcasted_iota(jnp.int32, (span, rows), 1)
        band = (rel >= 0) & (rel <= 2 * WINDOW)
        for b in range(blocks):
            pos = key + (offset + b * rows - WINDOW)
            ok = band & (pos >= 0) & (pos < limit)
            bias[b] = jnp.where(ok, 0.0, MASK_VALUE)

    pad[0:WINDOW] = b_ref[0]
    pad[WINDOW : WINDOW + tok] = kv_ref[0]
    pad[WINDOW + tok : length] = a_ref[0]
    lane = lax.broadcasted_iota(jnp.int32, (length, LANES), 1)
    for h in range(heads):
        at = (h * HEAD_DIM) % LANES
        src = (h // group) * HEAD_DIM
        chunk = src // LANES * LANES
        part = pad[:, chunk : chunk + LANES].astype(F32)
        shift = (at - src % LANES) % LANES
        if shift:
            part = pltpu.roll(part, shift, 1)
        keep = (lane >= at) & (lane < at + HEAD_DIM)
        kx[h] = jnp.where(keep, part, 0.0).astype(BF16)
    first = kw // LANES * LANES
    for c in range(first, kv2, LANES):
        vt[c - first : c - first + LANES] = (
            pad[:, c : c + LANES].astype(F32).T.astype(BF16)
        )

    for b in range(blocks):
        r0 = b * rows
        dest, off = r0 // share, r0 % share
        for pair in range(qw // LANES):
            q = q_ref[0, r0 : r0 + rows, pair * LANES : (pair + 1) * LANES]
            outs = []
            for h in range(pair * 2, pair * 2 + 2):
                sink = sink_ref[h]
                s = lax.dot_general(
                    kx[h, r0 : r0 + span],
                    q,
                    (((1,), (1,)), ((), ())),
                    preferred_element_type=F32,
                )
                s = s + bias[b]
                top = jnp.maximum(jnp.max(s, axis=0, keepdims=True), sink)
                e = jnp.exp(s - top)
                total = jnp.sum(e, axis=0, keepdims=True) + jnp.exp(sink - top)
                v0 = kw + (h // group) * HEAD_DIM - first
                o = jnp.dot(
                    vt[v0 : v0 + HEAD_DIM, r0 : r0 + span],
                    e.astype(BF16),
                    preferred_element_type=F32,
                )
                outs.append(o / total)
                l_ref[0, h : h + 1, r0 : r0 + rows] = top + jnp.log(total)
            both = jnp.concatenate(outs, axis=0).T
            o_ref[dest, 0, off : off + rows, pair * LANES : (pair + 1) * LANES] = (
                both.astype(BF16)
            )


def attention(q, kv, before, after, sink, tp, start, seqs):
    _, tok, qw = q.shape
    kv2 = kv.shape[2]
    kw = kv2 // 2
    heads = qw // HEAD_DIM
    group = heads // (kw // HEAD_DIM)
    share = tok // tp
    rows = math.gcd(share, 256)
    length = tok + 2 * WINDOW
    span = rows + 2 * WINDOW
    first = kw // LANES * LANES
    return pl.pallas_call(
        functools.partial(attn_kernel, group),
        grid=(seqs,),
        in_specs=[
            pl.BlockSpec(memory_space=pltpu.SMEM),
            pl.BlockSpec((1, tok, qw), lambda s: (s + start, 0, 0)),
            pl.BlockSpec((1, tok, kv2), lambda s: (s + start, 0, 0)),
            pl.BlockSpec((1, WINDOW, kv2), lambda s: (s + start, 0, 0)),
            pl.BlockSpec((1, WINDOW, kv2), lambda s: (s + start, 0, 0)),
        ],
        out_specs=[
            pl.BlockSpec((tp, 1, share, qw), lambda s: (0, s, 0, 0)),
            pl.BlockSpec((1, heads, tok), lambda s: (s, 0, 0)),
        ],
        out_shape=[
            jax.ShapeDtypeStruct((tp, seqs, share, qw), BF16),
            jax.ShapeDtypeStruct((seqs, heads, tok), F32),
        ],
        scratch_shapes=[
            pltpu.VMEM((length, kv2), BF16),
            pltpu.VMEM((heads, length, LANES), BF16),
            pltpu.VMEM((kv2 - first, length), BF16),
            pltpu.VMEM((tok // rows, span, rows), F32),
        ],
        compiler_params=params("arbitrary"),
        cost_estimate=cost(
            2000 * seqs * tok * qw, 8 * seqs * tok * qw, seqs * heads * tok * span
        ),
        name="attention",
    )(sink, q, kv, before, after)


def out_kernel(c_ref, g_ref, w_ref, *rest):
    *a_refs, o_ref, x = rest
    tp, seqs, share, ch = c_ref.shape
    size, qw = a_refs[0].shape[1], a_refs[0].shape[3]
    step = ch + qw

    @pl.when(pl.program_id(0) == 0)
    def _():
        for s in range(seqs):
            parts = [c_ref[t, s].astype(F32) for t in range(tp)]
            mean = sum(p.sum(-1, keepdims=True) for p in parts) / (tp * ch)
            parts = [p - mean for p in parts]
            var = sum((p * p).sum(-1, keepdims=True) for p in parts) / (tp * ch)
            inv = lax.rsqrt(var + EPSILON)
            r = slice(s * share, (s + 1) * share)
            for t in range(tp):
                v = parts[t] * inv * g_ref[t].astype(F32)
                x[r, t * step : t * step + ch] = jax.nn.silu(v).astype(BF16)
                x[r, t * step + ch : (t + 1) * step] = a_refs[s // size][t, s % size]

    w = w_ref[0].reshape(tp * step, w_ref.shape[3])
    y = jnp.dot(x[...], w, preferred_element_type=F32).astype(BF16)
    o_ref[...] = y.reshape(o_ref.shape)


def out_proj(conv_tok, attn_parts, gain, weights):
    tp, seqs, share, ch = conv_tok.shape
    attn_shape = attn_parts[0].shape
    sp, _, depth, cols = weights.shape
    return pl.pallas_call(
        out_kernel,
        grid=(sp,),
        in_specs=[
            pl.BlockSpec((tp, seqs, share, ch), lambda j: (0, 0, 0, 0)),
            pl.BlockSpec((tp, 1, ch), lambda j: (0, 0, 0)),
            pl.BlockSpec((1, tp, depth, cols), lambda j: (j, 0, 0, 0)),
        ]
        + [pl.BlockSpec(attn_shape, lambda j: (0, 0, 0, 0))] * len(attn_parts),
        out_specs=pl.BlockSpec((seqs, share, cols), lambda j: (0, 0, j)),
        out_shape=jax.ShapeDtypeStruct((seqs, share, sp * cols), BF16),
        scratch_shapes=[pltpu.VMEM((seqs * share, tp * depth), BF16)],
        compiler_params=params("arbitrary"),
        cost_estimate=cost(
            2 * seqs * share * tp * depth * sp * cols, 2 * sp * tp * depth * cols
        ),
        name="out_proj",
    )(conv_tok, gain, weights, *attn_parts)


def on_device(
    tokens,
    norm_gain,
    conv_value_weight,
    conv_gate_weight,
    query_weight,
    key_weight,
    value_weight,
    conv_taps,
    conv_gain,
    sink_logit,
    out_conv_weight,
    out_attn_weight,
):
    seqs, tok, width = tokens.shape
    tp, sp = lax.axis_size("tp"), lax.axis_size("sp")
    ch = conv_value_weight.shape[1]
    qw, kw = query_weight.shape[1], key_weight.shape[1]

    in_w = lax.all_gather(
        jnp.concatenate(
            [conv_value_weight, conv_gate_weight, query_weight, key_weight, value_weight], 1
        ),
        "sp",
        axis=0,
        tiled=True,
    )
    out_w = lax.all_gather(
        jnp.concatenate([out_conv_weight, out_attn_weight], 0),
        ("sp", "tp"),
        axis=0,
        tiled=True,
    ).reshape(sp, tp, ch + qw, out_conv_weight.shape[1])
    gain = lax.all_gather(conv_gain.reshape(1, 1, ch), "tp", axis=0, tiled=True)

    floats = tokens.astype(F32)
    row_mean = floats.mean(-1, keepdims=True)
    centred = floats - row_mean
    variance = jnp.mean(centred * centred, -1, keepdims=True)
    normed = (centred * lax.rsqrt(variance + EPSILON) * norm_gain.astype(F32)).astype(BF16)
    normed = normed.reshape(seqs * tok, width)

    half = HEAD_DIM // 2
    lane = jnp.arange(LANES)
    inverse = ROPE_BASE ** (-(lane % half).astype(F32) / half)
    positions = (lax.axis_index("sp") * tok + jnp.arange(tok, dtype=jnp.int32)).astype(F32)
    angles = positions[:, None] * inverse[None, :]
    cos = jnp.cos(angles)
    sin = jnp.sin(angles) * jnp.where(lane % HEAD_DIM < half, -1.0, 1.0)[None, :]

    gated, q, kv = projections(normed, in_w, cos, sin, ch, qw, kw)
    gated = gated.reshape(seqs, tok, ch)
    q, kv = q.reshape(seqs, tok, qw), kv.reshape(seqs, tok, 2 * kw)
    halo = -(-(conv_taps.shape[0] // 2) // 16) * 16
    before, after = ring_halo(gated, halo)
    kv_before, kv_after = ring_halo(kv, WINDOW)
    filtered = depthwise(gated, before, after, conv_taps.astype(F32), tp)
    conv_tok = lax.all_to_all(filtered, "tp", split_axis=0, concat_axis=0, tiled=True)

    attn_parts, totals = [], []
    count = math.gcd(seqs, 2)
    size = seqs // count
    for part in range(count):
        out, total = attention(
            q, kv, kv_before, kv_after, sink_logit, tp, part * size, size
        )
        attn_parts.append(
            lax.all_to_all(out, "tp", split_axis=0, concat_axis=0, tiled=True)
        )
        totals.append(total)
    log_total = jnp.concatenate(totals, axis=0)

    mixed = out_proj(conv_tok, attn_parts, gain, out_w)
    return (mixed, log_total)


def solution(mesh):
    placed = (
        P(None, "sp", None),
        P(),
        P("sp", "tp"),
        P("sp", "tp"),
        P("sp", "tp"),
        P("sp", "tp"),
        P("sp", "tp"),
        P(None, "tp"),
        P("tp"),
        P("tp"),
        P("tp", "sp"),
        P("tp", "sp"),
    )
    return jax.shard_map(
        on_device,
        mesh=mesh,
        in_specs=placed,
        out_specs=(P(None, ("sp", "tp"), None), P(None, "tp", "sp")),
        check_vma=False,
    )
```
